32 devices in a mesh: fs: 16 (over z, y, x), tp: 2 (over core).
Axes of the slice: x: 2, y: 2, z: 4, core: 2. Of those that a mesh axis runs over, the one named last changes fastest.
Arguments:
- tokens: bfloat16 [8192, 2048], P('fs', 'tp'), may hold values from -24 to 24
- u_weight: bfloat16 [2048, 1024], P('fs', 'tp'), may hold values from -0.125 to 0.125
- v_weight: bfloat16 [2048, 1024], P('fs', 'tp'), may hold values from -0.125 to 0.125
- sg_gain: float32 [1024], P('tp'), may hold values from 0.1 to 1.9
- spatial_weight: bfloat16 [8, 128, 128], P('tp'), may hold values from -0.5 to 0.5
- spatial_bias: float32 [8, 128], P('tp'), may hold values from 0.1 to 1.9
- out_weight: bfloat16 [1024, 2048], P('tp', 'fs'), may hold values from -0.1875 to 0.1875
- gain_one: float32 [2048], P('tp'), may hold values from 0.1 to 1.9
- gate_weight: bfloat16 [2048, 5632], P('fs', 'tp'), may hold values from -0.125 to 0.125
- up_weight: bfloat16 [2048, 5632], P('fs', 'tp'), may hold values from -0.125 to 0.125
- down_weight: bfloat16 [5632, 2048], P('tp', 'fs'), may hold values from -0.078125 to 0.078125
- gain_two: float32 [2048], P('tp'), may hold values from 0.1 to 1.9
Outputs:
- layer_out: bfloat16 [8192, 2048], P('fs', 'tp')
The draws below stay inside these ranges and needn't reach their ends.
All inputs are finite; a program needn't handle non-finite values.
Results may differ from the reference program's by a relative error of at most 0.014.
Values may be sent and summed in bfloat16 or wider, within the bound.
A program may use at most 128 MiB of HBM per device.

```python
import math
import jax
import jax.numpy as jnp
from jax import lax

D = 2048
FF = 5632
GROUPS = 8
GROUP_DIM = 128
BLOCK = 128
D_SG = 1024
TOKENS = 8192
N_TP = 2


def draw_tokens(key, part):
    first_key, second_key, third_key = jax.random.split(jax.random.fold_in(key, 11), 3)
    width = D // 16
    scales = jnp.exp(jax.random.uniform(second_key, (16,), jnp.float32, -math.log(4.0), math.log(4.0)))
    base = jax.random.normal(first_key, (TOKENS, D), jnp.float32)
    base = jnp.clip(base, -6.0, 6.0)
    return (base * jnp.repeat(scales, width)[None, :]).astype(jnp.bfloat16)


def steps_of(key, shape, pieces, least, high):
    factor_of, own = 1.0, jax.random.fold_in(key, 6)
    for position, blocks in pieces:
        draws = jnp.exp(jax.random.uniform(jax.random.fold_in(own, position), (blocks,), jnp.float32, least / len(pieces), high / len(pieces)))
        factor_of = factor_of * jnp.repeat(draws, shape[position] // blocks).reshape([-1 if axis == position else 1 for axis in range(len(shape))])
    return factor_of


def bell_draw(rng, extent, deviation, most, shards=(), kind=jnp.bfloat16):
    entries = deviation * jax.random.normal(rng, extent, jnp.float32)
    if shards:
        entries = entries * steps_of(rng, extent, shards, -0.22, 0.18)
    return jnp.clip(entries, -most, most).astype(kind)


def setup_inputs(seed: int = 0) -> dict:
    seeds = jax.random.split(jax.random.key(seed), 13)
    tokens = draw_tokens(jax.random.fold_in(seeds[12], 71), 0)
    u_weight = bell_draw(seeds[1], (D, D_SG), D ** -0.5, 0.125, ((0, 16), (1, 2)))
    v_weight = bell_draw(seeds[2], (D, D_SG), D ** -0.5, 0.125, ((0, 16), (1, 2)))
    sg_gain = jnp.clip(1.0 + 0.18 * jax.random.normal(seeds[3], (D_SG,), jnp.float32), 0.1, 1.9)
    spatial_weight = bell_draw(seeds[4], (GROUPS, BLOCK, BLOCK), BLOCK ** -0.5, 0.5, ((0, 2),))
    spatial_bias = jnp.clip(1.0 + 0.18 * jax.random.normal(seeds[5], (GROUPS, BLOCK), jnp.float32), 0.1, 1.9)
    out_weight = bell_draw(seeds[6], (D_SG, D), D_SG ** -0.5, 0.1875, ((0, 2), (1, 16)))
    gain_one = jnp.clip(1.0 + 0.18 * jax.random.normal(seeds[7], (D,), jnp.float32), 0.1, 1.9)
    gate_weight = bell_draw(seeds[8], (D, FF), D ** -0.5, 0.125, ((0, 16), (1, 2)))
    up_weight = bell_draw(seeds[9], (D, FF), D ** -0.5, 0.125, ((0, 16), (1, 2)))
    down_weight = bell_draw(seeds[10], (FF, D), FF ** -0.5, 0.078125, ((0, 2), (1, 16)))
    gain_two = jnp.clip(1.0 + 0.18 * jax.random.normal(seeds[11], (D,), jnp.float32), 0.1, 1.9)
    return {"tokens": tokens, "u_weight": u_weight, "v_weight": v_weight, "sg_gain": sg_gain, "spatial_weight": spatial_weight, "spatial_bias": spatial_bias, "out_weight": out_weight, "gain_one": gain_one, "gate_weight": gate_weight, "up_weight": up_weight, "down_weight": down_weight, "gain_two": gain_two}


EPS = 1e-05
ALPHA = 2.0 ** 0.25

def norm_rows(vals, gain):
    count = vals.shape[1]
    mean = lax.optimization_barrier(jnp.sum(vals, axis=1, keepdims=True)) / count
    square = lax.optimization_barrier(jnp.sum(vals * vals, axis=1, keepdims=True)) / count
    return (vals - mean) * lax.rsqrt(square - mean * mean + EPS) * gain.astype(jnp.float32)[None, :]

def split_sum(left, weight):
    width = weight.shape[0] // N_TP
    total = jnp.zeros((left.shape[0], weight.shape[1]), jnp.float32)
    for index in range(N_TP):
        part = jnp.dot(left[:, index * width:(index + 1) * width], weight[index * width:(index + 1) * width], preferred_element_type=jnp.float32).astype(jnp.bfloat16)
        part = lax.optimization_barrier(part)
        total = total + part.astype(jnp.float32)
    return total.astype(jnp.bfloat16)

def reference(tokens, u_weight, v_weight, sg_gain, spatial_weight, spatial_bias, out_weight, gain_one, gate_weight, up_weight, down_weight, gain_two):
    gated = jax.nn.gelu(jnp.dot(tokens, u_weight, preferred_element_type=jnp.float32))
    valued = jax.nn.gelu(jnp.dot(tokens, v_weight, preferred_element_type=jnp.float32))
    normed = norm_rows(valued, sg_gain).astype(jnp.bfloat16)
    blocks = TOKENS // BLOCK
    shaped = normed.reshape(blocks, BLOCK, GROUPS, GROUP_DIM).astype(jnp.float32)
    lower = jnp.tril(jnp.ones((BLOCK, BLOCK), jnp.float32))
    masked = spatial_weight.astype(jnp.float32) * lower[None]
    mixed = jnp.einsum('gij,njgd->nigd', masked, shaped)
    mixed = mixed + spatial_bias.astype(jnp.float32).T[None, :, :, None]
    gated_out = (gated * mixed.reshape(TOKENS, D_SG)).astype(jnp.bfloat16)
    mix = split_sum(gated_out, out_weight)
    first = norm_rows(ALPHA * tokens.astype(jnp.float32) + mix.astype(jnp.float32), gain_one).astype(jnp.bfloat16)
    gate = jnp.dot(first, gate_weight, preferred_element_type=jnp.float32)
    upper = jnp.dot(first, up_weight, preferred_element_type=jnp.float32)
    hidden = (jax.nn.silu(gate) * upper).astype(jnp.bfloat16)
    ffn = split_sum(hidden, down_weight)
    layer_out = norm_rows(ALPHA * first.astype(jnp.float32) + ffn.astype(jnp.float32), gain_two)
    return layer_out.astype(jnp.bfloat16)
```

```python
import jax
import jax.numpy as jnp
from jax import lax
from jax.sharding import PartitionSpec as P

EPS = 1e-05
ALPHA = 2.0**0.25


def add_rows(left, piece):
    return jnp.dot(left, piece, preferred_element_type=jnp.float32)


def scaled_rows(vals, sums, gain, count):
    mean = sums[0][:, None] / count
    square = sums[1][:, None] / count
    return (vals - mean) * lax.rsqrt(square - mean * mean + EPS) * gain[None, :]


def chip_sizes(count):
    across = 2 if count % 2 == 0 else 1
    down = 2 if (count // across) % 2 == 0 else 1
    return count // (across * down), down, across


def shift(value, sizes, axis):
    count = sizes[0] * sizes[1] * sizes[2]
    stride = sizes[1] * sizes[2] if axis == 0 else (sizes[2] if axis == 1 else 1)
    pairs = []
    for source in range(count):
        place = (source // stride) % sizes[axis]
        pairs.append((source, source + ((place + 1) % sizes[axis] - place) * stride))
    return lax.ppermute(value, "fs", pairs)


def ring(value, sizes, axis, place):
    pieces = [value]
    for _ in range(sizes[axis] - 1):
        pieces.append(shift(pieces[-1], sizes, axis))
    return in_order(pieces, place)


def in_order(pieces, place):
    count = len(pieces)
    if count == 1:
        return pieces[0][None]
    held = jnp.zeros((count,) + pieces[0].shape, pieces[0].dtype)
    for step, piece in enumerate(pieces):
        start = lax.rem(place - step + count, count)
        held = lax.dynamic_update_slice_in_dim(held, piece[None], start, 0)
    return held


def gather_all(piece, sizes, places, order):
    held = piece
    for axis in order:
        held = ring(held, sizes, axis, places[axis])
    back = [order[::-1].index(axis) for axis in range(3)]
    rest = [3 + i for i in range(piece.ndim)]
    return jnp.transpose(held, back + rest)


def gather_share(weight, dim, sizes, places):
    across = sizes[2]
    width = weight.shape[dim] // across
    if across == 2:
        mine = lax.dynamic_slice_in_dim(weight, places[2] * width, width, dim)
        other = lax.dynamic_slice_in_dim(weight, (1 - places[2]) * width, width, dim)
        block = in_order([mine, shift(other, sizes, 2)], places[2])
    else:
        block = weight[None]
    count = sizes[0]
    pieces = [block]
    for _ in range(count - 1):
        pieces.append(shift(pieces[-1], sizes, 0))
    if sizes[1] == 1:
        return in_order(pieces, places[0])[:, None]
    held = jnp.zeros((count, 2) + block.shape, block.dtype)
    zeros = [0] * block.ndim
    for step, piece in enumerate(pieces):
        start = lax.rem(places[0] - step + count, count)
        other = shift(piece, sizes, 1)
        held = lax.dynamic_update_slice(held, piece[None, None], [start, places[1]] + zeros)
        held = lax.dynamic_update_slice(held, other[None, None], [start, 1 - places[1]] + zeros)
    return held


def on_device(
    tokens,
    u_weight,
    v_weight,
    sg_gain,
    spatial_weight,
    spatial_bias,
    out_weight,
    gain_one,
    gate_weight,
    up_weight,
    down_weight,
    gain_two,
):
    parts = lax.axis_size("tp")
    sizes = chip_sizes(lax.axis_size("fs"))
    index = lax.axis_index("fs")
    places = (index // (sizes[1] * sizes[2]), (index // sizes[2]) % sizes[1], index % sizes[2])
    whole = lax.all_gather(tokens, "tp", axis=1, tiled=True)
    rows = whole.shape[0]
    width_sg = u_weight.shape[1]

    def add_one(piece):
        return add_rows(whole, piece)

    pre_u = add_one(gather_all(u_weight, sizes, places, [0, 1, 2]).reshape(-1, width_sg))
    pre_v = add_one(gather_all(v_weight, sizes, places, [0, 2, 1]).reshape(-1, width_sg))
    gated = jax.nn.gelu(pre_u)
    valued = jax.nn.gelu(pre_v)
    stats = lax.psum((jnp.sum(valued, axis=1), jnp.sum(valued * valued, axis=1)), "tp")
    normed = scaled_rows(valued, stats, sg_gain, width_sg * parts).astype(jnp.bfloat16)
    groups_here = spatial_weight.shape[0]
    block = spatial_weight.shape[1]
    group_width = width_sg // groups_here
    shaped = normed.reshape(rows // block, block, groups_here, group_width)
    lower = jnp.tril(jnp.ones((block, block), jnp.bool_))
    masked = jnp.where(lower[None], spatial_weight, jnp.zeros_like(spatial_weight))
    mixed = jnp.einsum("gij,njgd->nigd", masked, shaped, preferred_element_type=jnp.float32)
    mixed = mixed + spatial_bias.T[None, :, :, None]
    gated_out = (gated * mixed.reshape(rows, width_sg)).astype(jnp.bfloat16)
    out_all = gather_all(out_weight, sizes, places, [0, 1, 2])
    out_all = out_all.reshape((-1,) + out_weight.shape)
    terms = jnp.einsum("tk,nkc->tnc", gated_out, out_all, preferred_element_type=jnp.float32)
    terms = terms.reshape(rows, -1)
    mix = lax.psum_scatter(terms.astype(jnp.bfloat16), "tp", scatter_dimension=1, tiled=True)
    resid = ALPHA * tokens.astype(jnp.float32) + mix.astype(jnp.float32)
    first_sums = lax.psum((jnp.sum(resid, axis=1), jnp.sum(resid * resid, axis=1)), "tp")
    first = scaled_rows(resid, first_sums, gain_one, resid.shape[1] * parts).astype(jnp.bfloat16)
    gate_all = gather_share(gate_weight, 1, sizes, places)
    gate_all = gate_all.reshape(-1, gate_all.shape[-1])
    up_all = gather_share(up_weight, 1, sizes, places)
    up_all = up_all.reshape(-1, up_all.shape[-1])
    down_all = gather_share(down_weight, 0, sizes, places)
    down_all = down_all.reshape((-1,) + down_all.shape[-2:])

    def feed(part):
        whole_part = lax.all_gather(part, "tp", axis=1, tiled=True)
        gate = add_rows(whole_part, gate_all)
        upper = add_rows(whole_part, up_all)
        return (jax.nn.silu(gate) * upper).astype(jnp.bfloat16)

    def project(hidden):
        made = jnp.einsum("tf,nfc->tnc", hidden, down_all, preferred_element_type=jnp.float32)
        made = made.reshape(rows, -1).astype(jnp.bfloat16)
        return lax.psum_scatter(made, "tp", scatter_dimension=1, tiled=True)

    if sizes[2] == 2:
        there = feed(shift(first, sizes, 2))
        here = feed(first)
        sent = shift(project(there), sizes, 2)
        ffn = project(here).astype(jnp.float32) + sent.astype(jnp.float32)
    else:
        ffn = project(feed(first))
    second = ALPHA * first.astype(jnp.float32) + ffn.astype(jnp.float32)
    last_sums = lax.psum((jnp.sum(second, axis=1), jnp.sum(second * second, axis=1)), "tp")
    return scaled_rows(second, last_sums, gain_two, second.shape[1] * parts).astype(jnp.bfloat16)


def solution(mesh):
    return jax.shard_map(
        on_device,
        mesh=mesh,
        in_specs=(
            P("fs", "tp"),
            P("fs", "tp"),
            P("fs", "tp"),
            P("tp"),
            P("tp", None, None),
            P("tp", None),
            P("tp", "fs"),
            P("tp"),
            P("fs", "tp"),
            P("fs", "tp"),
            P("tp", "fs"),
            P("tp"),
        ),
        out_specs=P("fs", "tp"),
        check_vma=False,
    )
```

```python
import jax
import jax.numpy as jnp
from jax import lax
from jax.sharding import PartitionSpec as P

EPS = 1e-05
ALPHA = 2.0**0.25


def add_rows(left, piece):
    return jnp.dot(left, piece, preferred_element_type=jnp.float32)


def scaled_rows(vals, sums, gain, count):
    mean = sums[0][:, None] / count
    square = sums[1][:, None] / count
    return (vals - mean) * lax.rsqrt(square - mean * mean + EPS) * gain[None, :]


def chip_sizes(count):
    across = 2 if count % 2 == 0 else 1
    down = 2 if (count // across) % 2 == 0 else 1
    return count // (across * down), down, across


def shift(value, sizes, axis, step=1):
    count = sizes[0] * sizes[1] * sizes[2]
    stride = sizes[1] * sizes[2] if axis == 0 else (sizes[2] if axis == 1 else 1)
    pairs = []
    for source in range(count):
        place = (source // stride) % sizes[axis]
        pairs.append((source, source + ((place + step) % sizes[axis] - place) * stride))
    return lax.ppermute(value, "fs", pairs)


def around(value, sizes, axis):
    if sizes[axis] == 4:
        near = shift(value, sizes, axis, 1)
        last = shift(value, sizes, axis, -1)
        return [value, near, shift(near, sizes, axis, 1), last]
    pieces = [value]
    for _ in range(sizes[axis] - 1):
        pieces.append(shift(pieces[-1], sizes, axis))
    return pieces


def ring(value, sizes, axis, place):
    return in_order(around(value, sizes, axis), place)


def other_core(value):
    return lax.ppermute(value, "tp", [(0, 1), (1, 0)])


def all_features(value):
    if lax.axis_size("tp") != 2:
        return lax.all_gather(value, "tp", axis=1, tiled=True)
    return jnp.concatenate(in_two(value, other_core(value), lax.axis_index("tp")), axis=1)


def in_two(mine, other, place):
    return [jnp.where(place == 0, mine, other), jnp.where(place == 0, other, mine)]


def sum_shares(terms):
    if lax.axis_size("tp") != 2:
        return lax.psum_scatter(terms, "tp", scatter_dimension=1, tiled=True)
    core = lax.axis_index("tp")
    half = terms.shape[1] // 2
    mine = lax.dynamic_slice_in_dim(terms, core * half, half, 1)
    sent = lax.dynamic_slice_in_dim(terms, (1 - core) * half, half, 1)
    return (mine.astype(jnp.float32) + other_core(sent).astype(jnp.float32)).astype(jnp.bfloat16)


def in_order(pieces, place):
    count = len(pieces)
    if count == 1:
        return pieces[0][None]
    held = jnp.zeros((count,) + pieces[0].shape, pieces[0].dtype)
    for step, piece in enumerate(pieces):
        start = lax.rem(place - step + count, count)
        held = lax.dynamic_update_slice_in_dim(held, piece[None], start, 0)
    return held


def gather_all(piece, sizes, places, order):
    held = piece
    for axis in order:
        held = ring(held, sizes, axis, places[axis])
    back = [order[::-1].index(axis) for axis in range(3)]
    rest = [3 + i for i in range(piece.ndim)]
    return jnp.transpose(held, back + rest)


def after(value, *others):
    return lax.optimization_barrier((value,) + others)[0]


def share_pieces(weight, dim, sizes, places, level, marks):
    across = sizes[2]
    width = weight.shape[dim] // across
    if across == 2:
        mine = lax.dynamic_slice_in_dim(weight, places[2] * width, width, dim)
        other = lax.dynamic_slice_in_dim(weight, (1 - places[2]) * width, width, dim)
        block = jnp.stack(in_two(mine, shift(other, sizes, 2), places[2]))
    else:
        block = weight[None]
    if sizes[0] != 4 or sizes[1] != 2:
        first = around(block, sizes, 0)
        return [[piece] if sizes[1] == 1 else [piece, shift(piece, sizes, 1)] for piece in first]
    if marks[0] is not None:
        block = after(block, marks[0])
    near, last = shift(block, sizes, 0, 1), shift(block, sizes, 0, -1)
    beside = shift(block if marks[0] is None else after(block, marks[1]), sizes, 1)
    near, last = after(near, marks[1]), after(last, marks[1])
    far = shift(near, sizes, 0)
    near_beside, last_beside = shift(near, sizes, 1), shift(last, sizes, 1)
    if level:
        far_beside = shift(after(near_beside, marks[2]), sizes, 0)
    else:
        far = after(far, marks[2])
        far_beside = shift(far, sizes, 1)
    return [[block, beside], [near, near_beside], [far, far_beside], [last, last_beside]]


def place_pieces(pieces, places):
    shape = pieces[0][0].shape
    count, down = len(pieces), len(pieces[0])
    held = jnp.zeros((count, down) + shape, pieces[0][0].dtype)
    for step, pair in enumerate(pieces):
        start = lax.rem(places[0] - step + count, count)
        for turn, piece in enumerate(pair):
            spot = places[1] if turn == 0 else 1 - places[1]
            held = lax.dynamic_update_slice(held, piece[None, None], [start, spot] + [0] * len(shape))
    return held


def on_device(
    tokens,
    u_weight,
    v_weight,
    sg_gain,
    spatial_weight,
    spatial_bias,
    out_weight,
    gain_one,
    gate_weight,
    up_weight,
    down_weight,
    gain_two,
):
    parts = lax.axis_size("tp")
    sizes = chip_sizes(lax.axis_size("fs"))
    index = lax.axis_index("fs")
    places = (index // (sizes[1] * sizes[2]), (index // sizes[2]) % sizes[1], index % sizes[2])
    whole = all_features(tokens)
    rows = whole.shape[0]
    width_sg = u_weight.shape[1]

    def add_one(piece):
        return add_rows(whole, piece)

    pre_u = add_one(gather_all(u_weight, sizes, places, [0, 1, 2]).reshape(-1, width_sg))
    pre_v = add_one(gather_all(v_weight, sizes, places, [0, 2, 1]).reshape(-1, width_sg))
    gated = jax.nn.gelu(pre_u)
    valued = jax.nn.gelu(pre_v)
    stats = lax.psum((jnp.sum(valued, axis=1), jnp.sum(valued * valued, axis=1)), "tp")
    normed = scaled_rows(valued, stats, sg_gain, width_sg * parts).astype(jnp.bfloat16)
    groups_here = spatial_weight.shape[0]
    block = spatial_weight.shape[1]
    group_width = width_sg // groups_here
    shaped = normed.reshape(rows // block, block, groups_here, group_width)
    lower = jnp.tril(jnp.ones((block, block), jnp.bool_))
    masked = jnp.where(lower[None], spatial_weight, jnp.zeros_like(spatial_weight))
    mixed = jnp.einsum("gij,njgd->nigd", masked, shaped, preferred_element_type=jnp.float32)
    mixed = mixed + spatial_bias.T[None, :, :, None]
    gated_out = (gated * mixed.reshape(rows, width_sg)).astype(jnp.bfloat16)
    out_all = gather_all(out_weight, sizes, places, [0, 1, 2])
    out_all = out_all.reshape((-1,) + out_weight.shape)
    terms = jnp.einsum("tk,nkc->tnc", gated_out, out_all, preferred_element_type=jnp.float32)
    mix = sum_shares(terms.reshape(rows, -1).astype(jnp.bfloat16))
    resid = ALPHA * tokens.astype(jnp.float32) + mix.astype(jnp.float32)
    first_sums = lax.psum((jnp.sum(resid, axis=1), jnp.sum(resid * resid, axis=1)), "tp")
    first = scaled_rows(resid, first_sums, gain_one, resid.shape[1] * parts).astype(jnp.bfloat16)
    gate_pieces = share_pieces(gate_weight, 1, sizes, places, False, (None, normed, mix))
    up_pieces = share_pieces(up_weight, 1, sizes, places, True, (None, normed, mix))
    down_pieces = share_pieces(down_weight, 0, sizes, places, False, (normed, first, first))
    gate_all = place_pieces(gate_pieces, places)
    gate_all = gate_all.reshape(-1, gate_all.shape[-1])
    up_all = place_pieces(up_pieces, places)
    up_all = up_all.reshape(-1, up_all.shape[-1])
    def feed(part):
        whole_part = all_features(part)
        gate = add_rows(whole_part, gate_all)
        upper = add_rows(whole_part, up_all)
        return (jax.nn.silu(gate) * upper).astype(jnp.bfloat16)

    two = sizes[2] == 2
    if two:
        there = feed(shift(first, sizes, 2))
        here = feed(first)
        down_pieces = [[pair[0]] + [after(piece, there, here) for piece in pair[1:]] for pair in down_pieces]
    else:
        here = feed(first)
    down_all = place_pieces(down_pieces, places)
    down_all = down_all.reshape((-1,) + down_all.shape[-2:])

    def project(hidden):
        made = jnp.einsum("tf,nfc->tnc", hidden, down_all, preferred_element_type=jnp.float32)
        return sum_shares(made.reshape(rows, -1).astype(jnp.bfloat16))

    if two:
        there = project(there)
        sent = shift(there, sizes, 2)
        ffn = project(after(here, there)).astype(jnp.float32) + sent.astype(jnp.float32)
    else:
        ffn = project(here).astype(jnp.float32)
    second = ALPHA * first.astype(jnp.float32) + ffn.astype(jnp.float32)
    last_sums = lax.psum((jnp.sum(second, axis=1), jnp.sum(second * second, axis=1)), "tp")
    return scaled_rows(second, last_sums, gain_two, second.shape[1] * parts).astype(jnp.bfloat16)


def solution(mesh):
    return jax.shard_map(
        on_device,
        mesh=mesh,
        in_specs=(
            P("fs", "tp"),
            P("fs", "tp"),
            P("fs", "tp"),
            P("tp"),
            P("tp", None, None),
            P("tp", None),
            P("tp", "fs"),
            P("tp"),
            P("fs", "tp"),
            P("fs", "tp"),
            P("tp", "fs"),
            P("tp"),
        ),
        out_specs=P("fs", "tp"),
        check_vma=False,
    )
```
